1024 devices in a mesh: ep: 32 (over z, core), tp: 32 (over y, x).
Axes of the slice: x: 4, y: 8, z: 16, core: 2. Of those that a mesh axis runs over, the one named last changes fastest.
Arguments:
- tokens: bfloat16 [2048, 2048], P('ep', 'tp'), as said below
- mix_gain: float32 [2048], replicated, may hold values from 0.1 to 1.9
- w_in: bfloat16 [2048, 1024], P(None, 'tp'), may hold values from -0.125 to 0.125
- a_real: float32 [64, 64], P('tp'), may hold values from -1 to -0.1
- a_imag: float32 [64, 64], P('tp'), may hold values from -3.140625 to 3.140625
- log_step: float32 [64], P('tp'), may hold values from -3 to 0
- b_coef: float32 [2, 64, 64, 16], P(None, 'tp'), may hold values from -2.5 to 2.5
- output_coefficients: float32 [2, 64, 16, 64], P(None, 'tp'), may hold values from -1.25 to 1.25
- skip: float32 [1024], P('tp'), may hold values from -6 to 6
- w_out: bfloat16 [1024, 2048], P('tp'), may hold values from -0.1875 to 0.1875
- state: float32 [2, 2048, 64, 64], P(None, 'ep', 'tp'), may hold values from -6 to 6
- ffn_gain: float32 [2048], replicated, may hold values from 0.1 to 1.9
- w_gate: bfloat16 [64, 2048, 4096], P('ep', None, 'tp'), may hold values from -0.125 to 0.125
- w_up: bfloat16 [64, 2048, 4096], P('ep', None, 'tp'), may hold values from -0.125 to 0.125
- w_down: bfloat16 [64, 4096, 2048], P('ep', 'tp'), may hold values from -0.09375 to 0.09375
- expert_ids: int32 [2048, 2], P('ep'), may hold values from 0 to 63, all different within a row; in each aligned block of 64 rows (0 to 63, 64 to 127, ...) at most 4 rows name the same one
- route_weights: float32 [2048, 2], P('ep'), may hold values from 0.3 to 1
Outputs:
- out: bfloat16 [2048, 2048], P('ep', 'tp')
- new_state: float32 [2, 2048, 64, 64], P(None, 'ep', 'tp')
The draws below stay inside these ranges and needn't reach their ends.
Inputs may be any that keep to these rules, and one draw needn't show every extreme that they name: `expert_ids`: A token's 2 experts differ. Among the 64 rows of one index of ep no expert is named more than 4 times, a bound that some block reaches. `tokens`: feature scales differ along the model width.
All inputs are finite; a program needn't handle non-finite values.
Results may differ from the reference program's by a relative error of at most 0.007.
Values may be sent and summed in bfloat16 or wider, within the bound.
A program may use at most 32 MiB of HBM per device.

```python
import math
import jax
import jax.numpy as jnp
import numpy as np
from jax import lax

D = 2048
S5W = 1024
GROUP_CH = 16
STATE = 64
GROUPS = 64
FFE = 4096
TOPK = 2
EXPERTS = 64
SEQ_DEV = 64
SEQS = 2048
CAP = 4
N_EP = 32


def draw_tokens(key, part):
    base_key = jax.random.fold_in(key, 11)
    column = jnp.arange(D, dtype=jnp.float32) / D
    values = jax.random.normal(base_key, (SEQS, D), jnp.float32)
    scaled = values * jnp.exp(column * 1.1)[None, :]
    return scaled.astype(jnp.bfloat16)


def levels(rng, extent, cuts, low, high):
    def one(axis_at, parts):
        steps = jax.random.uniform(jax.random.fold_in(jax.random.fold_in(rng, 6), axis_at), (parts,), jnp.float32, low / len(cuts), high / len(cuts))
        return jnp.repeat(jnp.exp(steps), extent[axis_at] // parts).reshape((-1,) + (1,) * (len(extent) - axis_at - 1))

    loudness = one(*cuts[0])
    for cut in cuts[1:]:
        loudness = loudness * one(*cut)
    return loudness


def assign_block(key, own, number, rows, amount, top, most, lean):
    ranking = jax.random.permutation(key, amount)
    crowded, ordinary = shares(amount, rows * top, most, lean, True), shares(amount, rows * top, most, lean, False)
    places = jnp.arange(amount)

    def named(sizes, rotation):
        used = int((sizes > 0).sum())
        fixed = max(1, used // 4)
        moved = fixed + (places - fixed + rotation * (used - fixed)) % max(1, amount - fixed)
        return jnp.zeros((amount,), jnp.int32).at[ranking[jnp.where(places < fixed, places, moved)]].set(jnp.asarray(sizes, jnp.int32))

    sizes = jnp.where(number % 4 == 0, named(crowded, number // 4), named(ordinary, number - number // 4 - 1))
    mixed = jax.random.permutation(jax.random.fold_in(own, 3), amount)
    donor, receiver = mixed[0:amount // 2 * 2:2], mixed[1:amount // 2 * 2:2]
    room = jnp.minimum(sizes[donor] - 1, most - sizes[receiver]) // 2
    room = jnp.where((donor == ranking[0]) | (receiver == ranking[0]) | (sizes[receiver] == 0), 0, jnp.maximum(room, 0))
    moved = jax.random.randint(jax.random.fold_in(own, 4), (amount // 2,), 0, 1 << 20) % (room + 1)
    sizes = sizes.at[donor].add(-moved).at[receiver].add(moved)
    labels = jnp.searchsorted(jnp.cumsum(sizes), jnp.arange(rows * top), side="right").astype(jnp.int32)
    table = labels.reshape(top, rows).T
    table = table[jax.random.permutation(jax.random.fold_in(own, 1), rows)]
    rotation = jax.random.randint(jax.random.fold_in(own, 2), (rows, 1), 0, top)
    return jnp.take_along_axis(table, (jnp.arange(top)[None, :] + rotation) % top, axis=1)


def shares(number_of, total, reach, skew, full):
    loads = [(1 << 20) // math.isqrt(grade ** skew) + 1 for grade in range(1, number_of + 1)]
    largest = reach if full else min(reach, max(-(-total // number_of), total * loads[0] // sum(loads)))
    least = 1 if total - largest >= number_of - 1 else 0
    given, spare = [largest] + [least] * (number_of - 1), total - largest - least * (number_of - 1)
    while spare > 0:
        movable = [i for i in range(1, number_of) if given[i] < largest] or [i for i in range(1, number_of) if given[i] < reach]
        pool, remaining = sum([loads[i] for i in movable]), spare
        for i in movable:
            more = min(reach - given[i], max(1, remaining * loads[i] // pool), spare)
            given[i] = given[i] + more
            spare = spare - more
    return np.array(given)


def centred(stream_key, shape, spread, bound, cuts=(), held_as=jnp.bfloat16):
    values = spread * jax.random.normal(stream_key, shape, jnp.float32)
    if cuts:
        values = values * levels(stream_key, shape, cuts, -0.22, 0.18)
    return jnp.clip(values, -bound, bound).astype(held_as)


def setup_inputs(seed: int = 0) -> dict:
    keys = jax.random.split(jax.random.key(seed), 18)
    tokens = draw_tokens(jax.random.fold_in(keys[17], 71), 0)
    mix_gain = jnp.clip(1.0 + 0.18 * jax.random.normal(keys[1], (D,), jnp.float32), 0.1, 1.9)
    w_in = centred(keys[2], (D, S5W), D ** -0.5, 0.125, ((1, 32),))
    a_real = jnp.clip(-1.0 + 0.9 * jax.random.uniform(keys[3], (GROUPS, STATE), jnp.float32) ** levels(keys[3], (GROUPS, STATE), ((0, 32),), -0.2, 0.2), -1.0, -0.1)
    a_imag = jnp.clip(jax.random.uniform(keys[4], (GROUPS, STATE), jnp.float32, -3.140625, 3.140625), -3.140625, 3.140625)
    log_step = jnp.clip(-3.0 + 3.0 * jax.random.uniform(keys[5], (GROUPS,), jnp.float32) ** levels(keys[5], (GROUPS,), ((0, 32),), -0.2, 0.2), -3.0, 0.0)
    b_coef = centred(keys[6], (2, GROUPS, STATE, GROUP_CH), ((2 * GROUP_CH) ** -0.5), 2.5, ((1, 32),), jnp.float32)
    output_coefficients = centred(keys[7], (2, GROUPS, GROUP_CH, STATE), ((2 * STATE) ** -0.5), 1.25, ((1, 32),), jnp.float32)
    skip = centred(keys[8], (S5W,), 1.0, 6.0, ((0, 32),), jnp.float32)
    w_out = centred(keys[9], (S5W, D), S5W ** -0.5, 0.1875, ((0, 32),))
    state = centred(keys[10], (2, SEQS, GROUPS, STATE), 1.0, 6.0, ((1, 32), (2, 32)), jnp.float32)
    ffn_gain = jnp.clip(1.0 + 0.18 * jax.random.normal(keys[11], (D,), jnp.float32), 0.1, 1.9)
    w_gate = centred(keys[12], (EXPERTS, D, FFE), D ** -0.5, 0.125, ((0, 32), (2, 32)))
    w_up = centred(keys[13], (EXPERTS, D, FFE), D ** -0.5, 0.125, ((0, 32), (2, 32)))
    w_down = centred(keys[14], (EXPERTS, FFE, D), FFE ** -0.5, 0.09375, ((0, 32), (1, 32)))
    expert_ids_keys = jax.random.split(jax.random.fold_in(keys[15], 1), SEQS // SEQ_DEV)
    expert_ids_turns = jax.random.permutation(jax.random.fold_in(keys[15], 3), SEQS // SEQ_DEV)
    expert_ids = jax.vmap(lambda own, number: assign_block(jax.random.fold_in(keys[15], 2), own, number, SEQ_DEV, EXPERTS, TOPK, CAP, 2))(expert_ids_keys, expert_ids_turns).reshape((SEQS, TOPK))
    route_weights = jnp.clip(0.3 + 0.7 * jax.random.uniform(keys[16], (SEQS, TOPK), jnp.float32) ** levels(keys[16], (SEQS, TOPK), ((0, 32),), -0.2, 0.2), 0.3, 1.0)
    return {"tokens": tokens, "mix_gain": mix_gain, "w_in": w_in, "a_real": a_real, "a_imag": a_imag, "log_step": log_step, "b_coef": b_coef, "output_coefficients": output_coefficients, "skip": skip, "w_out": w_out, "state": state, "ffn_gain": ffn_gain, "w_gate": w_gate, "w_up": w_up, "w_down": w_down, "expert_ids": expert_ids, "route_weights": route_weights}


epsilon = 1e-06
highest_precision = lax.Precision.HIGHEST

def rms_norm(values, gain):
    scaled = values * lax.rsqrt(lax.optimization_barrier(jnp.mean(values * values, axis=-1, keepdims=True)) + epsilon)
    return scaled * gain.astype(jnp.float32)

def state_update(drive, a_real, a_imag, log_step, b_coef, output_coefficients, skip, state):
    count = drive.shape[0]
    groups = a_real.shape[0]
    drive_float = drive.astype(jnp.float32)
    grouped = drive_float.reshape(count, groups, -1)
    step_size = jnp.exp(log_step)[:, None]
    magnitude = jnp.exp(step_size * a_real)
    decay_re = magnitude * jnp.cos(step_size * a_imag)
    decay_imaginary = magnitude * jnp.sin(step_size * a_imag)
    denominator = a_real * a_real + a_imag * a_imag
    shifted = decay_re - 1.0
    factor_re = (shifted * a_real + decay_imaginary * a_imag) / denominator
    factor_im = (decay_imaginary * a_real - shifted * a_imag) / denominator
    coef_re = factor_re[..., None] * b_coef[0] - factor_im[..., None] * b_coef[1]
    coefficient_imaginary = factor_re[..., None] * b_coef[1] + factor_im[..., None] * b_coef[0]
    push_re = jnp.einsum('gpc,sgc->sgp', coef_re, grouped, precision=highest_precision)
    push_im = jnp.einsum('gpc,sgc->sgp', coefficient_imaginary, grouped, precision=highest_precision)
    state_real = decay_re * state[0] - decay_imaginary * state[1] + push_re
    state_imaginary = decay_re * state[1] + decay_imaginary * state[0] + push_im
    state_readout = jnp.einsum('amz,daz->dam', output_coefficients[0], state_real, precision=highest_precision) - jnp.einsum('amz,daz->dam', output_coefficients[1], state_imaginary, precision=highest_precision)
    mixed = state_readout.reshape(count, -1) + skip * drive_float
    return (jax.nn.gelu(mixed).astype(jnp.bfloat16), jnp.stack([state_real, state_imaginary]))

def slot_table(expert_ids, experts, capacity):
    flat_ids = expert_ids.reshape(-1).astype(jnp.int32)
    onehot = (flat_ids[:, None] == jnp.arange(experts, dtype=jnp.int32)[None, :]).astype(jnp.int32)
    ranks = jnp.cumsum(onehot, axis=0) - 1
    slot_rank = lax.optimization_barrier(jnp.sum(onehot * ranks, axis=1))
    slots = flat_ids * capacity + slot_rank
    return (slots[:, None] == jnp.arange(experts * capacity, dtype=jnp.int32)[None, :]).astype(jnp.float32)

def reference(tokens, mix_gain, w_in, a_real, a_imag, log_step, b_coef, output_coefficients, skip, w_out, state, ffn_gain, w_gate, w_up, w_down, expert_ids, route_weights):
    tok_float = tokens.astype(jnp.float32)
    normed = rms_norm(tok_float, mix_gain).astype(jnp.bfloat16)
    drive = jnp.dot(normed, w_in, preferred_element_type=jnp.float32).astype(jnp.bfloat16)
    mixed, new_state = state_update(drive, a_real, a_imag, log_step, b_coef, output_coefficients, skip, state)
    resid = (tok_float + jnp.dot(mixed, w_out, preferred_element_type=jnp.float32)).astype(jnp.bfloat16)
    normed2 = rms_norm(resid.astype(jnp.float32), ffn_gain).astype(jnp.bfloat16)
    placed = jax.vmap(lambda block_ids: slot_table(block_ids, EXPERTS, CAP))(expert_ids.reshape(N_EP, SEQ_DEV, TOPK))
    repeated = jnp.repeat(normed2.reshape(N_EP, SEQ_DEV, D), TOPK, axis=1).astype(jnp.float32)
    buffer = jnp.einsum('nrs,nrd->nsd', placed, repeated, precision=highest_precision).astype(jnp.bfloat16)
    by_expert = buffer.reshape(N_EP, EXPERTS, CAP, D).transpose(1, 0, 2, 3)

    def one_expert(operands):
        slot_rows, gate_weight_matrix, weight_up, weight_down = operands
        flat_rows = slot_rows.reshape(-1, D)
        gate_vals = jnp.dot(flat_rows, gate_weight_matrix, preferred_element_type=jnp.float32)
        up_vals = jnp.dot(flat_rows, weight_up, preferred_element_type=jnp.float32)
        hidden = (jax.nn.silu(gate_vals) * up_vals).astype(jnp.bfloat16)
        result = jnp.dot(hidden, weight_down, preferred_element_type=jnp.float32).astype(jnp.bfloat16)
        return result.reshape(N_EP, CAP, D)
    results = lax.map(one_expert, (by_expert, w_gate, w_up, w_down))
    results = results.transpose(1, 0, 2, 3).reshape(N_EP, EXPERTS * CAP, D).astype(jnp.float32)
    weighted = placed * route_weights.reshape(N_EP, SEQ_DEV * TOPK)[..., None]
    combined = jnp.einsum('nrs,nsd->nrd', weighted, results, precision=highest_precision)
    combined = combined.reshape(SEQS, TOPK, D).sum(axis=1)
    out = (resid.astype(jnp.float32) + combined).astype(jnp.bfloat16)
    return (out, new_state)
```

```python
import jax
import jax.numpy as jnp
from jax import lax
from jax.experimental import pallas as pl
from jax.experimental.pallas import tpu as pltpu
from jax.sharding import PartitionSpec as P

EPS = 1e-06
HI = lax.Precision.HIGHEST
MESH = pl.DeviceIdType.MESH
NT = (((1,), (1,)), ((), ()))
TN = (((0,), (0,)), ((), ()))
F32 = jnp.float32
BF16 = jnp.bfloat16
NX, NY = 4, 8
TP, EP = 32, 32
NEAR = (0, 1, 7, 2, 6, 3, 5, 4)
FAR = (4, 3, 5, 2, 6, 1, 7, 0)


def iota(shape, dim):
    return lax.broadcasted_iota(jnp.int32, shape, dim)


def lo_lanes(rows, lanes=128):
    return iota((rows, lanes), 1) % 128 < 64


def swap(x):
    return pltpu.roll(x, 64, axis=x.ndim - 1)


def far_first(i):
    return 16 + ((i + 1) // 2) * (2 * (i % 2) - 1) * -1


def body(
    tok_ref, gain1_ref, win_hbm, ar_ref, ai_ref, ls_ref, b_ref, oc_ref, skip_ref, wout_ref,
    state_ref, gain2_ref, wg_hbm, wu_hbm, wd_hbm, ids_ref, rw_ref,
    out_ref, ns_ref,
    ta, ma, ws, wo, zs, zr, xf, yf, ro, rl, rr, ry, qs, qr, win2, wi, wdr, wd2,
    gd1, gd2, seltv, wtv, tokd,
    load_sem, sa, sw, sm, sz, sx, se, sq, ra, rw_sem, rm, rz, rq, rdy, rdl, rdr, rdo,
    reo, rel, rer, rey,
):
    t = lax.axis_index("tp")
    e = lax.axis_index("ep")
    y = t // NX
    x = t % NX
    xp = lax.rem(x + 1, NX)
    xm = lax.rem(x + NX - 1, NX)
    xo = lax.rem(x + 2, NX)

    loads = [
        pltpu.make_async_copy(win_hbm, win2.at[:, 0], load_sem.at[0]),
        pltpu.make_async_copy(win_hbm, win2.at[:, 1], load_sem.at[1]),
        pltpu.make_async_copy(wd_hbm, wdr, load_sem.at[2]),
    ]
    for j in range(2):
        loads.append(
            pltpu.make_async_copy(wg_hbm.at[j], wi.at[:, j, :, pl.ds(0, 128)], load_sem.at[3 + j])
        )
        loads.append(
            pltpu.make_async_copy(wu_hbm.at[j], wi.at[:, j, :, pl.ds(128, 128)], load_sem.at[5 + j])
        )
    barrier = pltpu.get_barrier_semaphore()

    def greet(i, c):
        d = far_first(i)
        pl.semaphore_signal(
            barrier, inc=1, device_id={"ep": lax.rem(e + d, EP)}, device_id_type=MESH
        )
        pl.semaphore_signal(
            barrier, inc=1, device_id={"tp": lax.rem(t + d, TP)}, device_id_type=MESH
        )
        return c

    lax.fori_loop(0, 31, greet, 0)
    for c in loads:
        c.start()

    tok = tok_ref[...]
    spread = (iota((64, 128), 1) % 64 == iota((64, 128), 0)).astype(F32)
    lo64 = lo_lanes(64)
    spread_lo = jnp.where(lo64, spread, 0.0).astype(BF16)
    spread_hi = jnp.where(lo64, 0.0, spread).astype(BF16)
    packed = jnp.dot(tok[0:32], spread_lo, preferred_element_type=F32) + jnp.dot(
        tok[32:64], spread_hi, preferred_element_type=F32
    )
    ta[t] = packed.astype(BF16)
    tokd[...] = jnp.dot(tok, spread.astype(BF16), preferred_element_type=F32)

    lo16 = lo_lanes(16)
    for k in range(16):
        blk = wout_ref[:, k * 128 : (k + 1) * 128].astype(F32)
        top, bot = blk[0:16], blk[16:32]
        ws[2 * k] = jnp.where(lo16, top, swap(bot)).astype(BF16)
        ws[2 * k + 1] = jnp.where(lo16, swap(top), bot).astype(BF16)
    wo[t] = ws[t]

    pl.semaphore_wait(barrier, 62)

    def to_tp(src, dst, send, recv):
        def one(i, c):
            dest = lax.rem(t + far_first(i), TP)
            pltpu.make_async_remote_copy(
                src_ref=src(dest), dst_ref=dst, send_sem=send, recv_sem=recv,
                device_id={"tp": dest}, device_id_type=MESH,
            ).start()
            return c

        lax.fori_loop(0, 31, one, 0)

    def to_ep(src, dst, send, recv):
        def one(i, c):
            dest = lax.rem(e + far_first(i), EP)
            pltpu.make_async_remote_copy(
                src_ref=src.at[dest], dst_ref=dst.at[e], send_sem=send, recv_sem=recv,
                device_id={"ep": dest}, device_id_type=MESH,
            ).start()
            return c

        lax.fori_loop(0, 31, one, 0)

    def all_of(ref, send, recv):
        r = ref.at[pl.ds(0, 31)]
        return pltpu.make_async_remote_copy(
            src_ref=r, dst_ref=r, send_sem=send, recv_sem=recv,
            device_id={"tp": lax.rem(t + 1, TP)}, device_id_type=MESH,
        )

    to_tp(lambda d: ta.at[t], ta.at[t], sa, ra)
    to_tp(lambda d: ws.at[d], wo.at[t], sw, rw_sem)

    ids = ids_ref[...]
    rw = rw_ref[...]
    lane = iota((64, 128), 1)
    id0, id1 = ids[:, 0:1], ids[:, 1:2]
    w0, w1 = rw[:, 0:1], rw[:, 1:2]
    below = (iota((64, 64), 1) < iota((64, 64), 0)).astype(F32).astype(BF16)
    sels = []
    for j in range(2):
        named = 2 * (lane // 4) + j
        hit0 = (id0 == named).astype(F32)
        hit1 = (id1 == named).astype(F32)
        hit = hit0 + hit1
        rank = jnp.dot(below, hit.astype(BF16), preferred_element_type=F32)
        here = (rank.astype(jnp.int32) == lane % 4).astype(F32)
        sels.append(hit * here)
        wtv[j] = (hit0 * w0 + hit1 * w1) * here
    seltv[...] = jnp.concatenate(sels, axis=0).T.astype(BF16)

    for src, dst in ((gain1_ref, gd1), (gain2_ref, gd2)):
        g = src[...]
        s = swap(g)
        lo = lo_lanes(16)
        dst[0] = jnp.where(lo, g, s)
        dst[1] = jnp.where(lo, s, g)

    loads[2].wait()
    lo128 = lo_lanes(128)
    for k in range(16):
        for j in range(2):
            blk = wdr[j, :, k * 128 : (k + 1) * 128].astype(F32)
            rolled = swap(blk)
            even, odd = (blk, rolled) if j == 0 else (rolled, blk)
            keep = lo128 if j == 0 else jnp.logical_not(lo128)
            for tt, piece in ((2 * k, even), (2 * k + 1, odd)):
                pos = (tt % NX) * NY + tt // NX
                wd2[pos, j * 128 : (j + 1) * 128, :] = jnp.where(keep, piece, 0.0).astype(BF16)
    for i in (0, 1, 3, 4, 5, 6):
        loads[i].wait()

    all_of(ta, sa, ra).wait_recv()
    lo32 = lo_lanes(32)
    acc = jnp.zeros((32, 128), F32)
    for k in range(TP):
        v = ta[k].astype(F32)
        acc = acc + v * v
    s0 = jnp.sum(jnp.where(lo32, acc, 0.0), axis=1, keepdims=True)
    s1 = jnp.sum(jnp.where(lo32, 0.0, acc), axis=1, keepdims=True)
    scale = jnp.where(
        lo32, lax.rsqrt(s0 / 2048.0 + EPS), lax.rsqrt(s1 / 2048.0 + EPS)
    )
    blocks = []
    for k in range(TP):
        v = ta[k].astype(F32) * scale * gd1[k % 2, k // 2 : k // 2 + 1, :]
        blocks.append(
            jnp.concatenate(
                [jnp.where(lo32, v, 0.0).astype(BF16), jnp.where(lo32, 0.0, v).astype(BF16)], axis=0
            )
        )
    drive = jnp.dot(
        jnp.concatenate(blocks, axis=1), win2[...].reshape(4096, 32), preferred_element_type=F32
    )
    drive = drive.astype(BF16).astype(F32)

    readout = skip_ref[...] * drive
    zeros16 = jnp.zeros((16, 64), F32)
    for g in range(2):
        step = jnp.exp(jnp.full((1, 64), ls_ref[g], F32))
        ar, ai = ar_ref[g : g + 1, :], ai_ref[g : g + 1, :]
        mag = jnp.exp(step * ar)
        dr, di = mag * jnp.cos(step * ai), mag * jnp.sin(step * ai)
        den = ar * ar + ai * ai
        sh = dr - 1.0
        fr, fi = (sh * ar + di * ai) / den, (di * ar - sh * ai) / den
        u = drive[:, g * 16 : (g + 1) * 16]
        q0 = lax.dot_general(u, b_ref[0, g], NT, precision=HI, preferred_element_type=F32)
        q1 = lax.dot_general(u, b_ref[1, g], NT, precision=HI, preferred_element_type=F32)
        p0, p1 = state_ref[0, :, g, :], state_ref[1, :, g, :]
        n0 = dr * p0 - di * p1 + (fr * q0 - fi * q1)
        n1 = dr * p1 + di * p0 + (fr * q1 + fi * q0)
        ns_ref[0, :, g, :] = n0
        ns_ref[1, :, g, :] = n1
        order = (lambda o: [o, zeros16]) if g == 0 else (lambda o: [zeros16, o])
        c0 = jnp.concatenate(order(oc_ref[0, g]), axis=0)
        c1 = jnp.concatenate(order(oc_ref[1, g]), axis=0)
        readout = readout + (
            lax.dot_general(n0, c0, NT, precision=HI, preferred_element_type=F32)
            - lax.dot_general(n1, c1, NT, precision=HI, preferred_element_type=F32)
        )
    mixed = jax.nn.gelu(readout)
    first = iota((64, 32), 1) < 16
    stacked = jnp.concatenate(
        [jnp.where(first, mixed, 0.0), jnp.where(first, 0.0, mixed)], axis=0
    ).astype(BF16)
    pick = (iota((16, 32), 1) % 16 == iota((16, 32), 0)).astype(F32).astype(BF16)
    ma[t] = lax.dot_general(pick, stacked, NT, preferred_element_type=F32).astype(BF16)
    to_tp(lambda d: ma.at[t], ma.at[t], sm, rm)

    all_of(wo, sw, rw_sem).wait_recv()
    all_of(ma, sm, rm).wait_recv()
    prod = lax.dot_general(
        ma[...].reshape(512, 128), wo[...].reshape(512, 128), TN, preferred_element_type=F32
    )
    half = jnp.where(lo64, prod[0:64], prod[64:128])
    resid = (tokd[...] + (half + swap(half))).astype(BF16)
    resid_f = resid.astype(F32)
    tokd[...] = resid_f

    zero = jnp.zeros((64, 128), F32)
    diag = jnp.concatenate(
        [jnp.where(lo64, resid_f, zero), jnp.where(lo64, zero, resid_f)], axis=0
    ).astype(BF16)
    sent = jnp.dot(seltv[...], diag, preferred_element_type=F32)
    ZPACK(zs, sent)
    zr[e] = zs[e]
    to_ep(zs, zr, sz, rz)
    all_of(zr, sz, rz).wait_recv()
    xf[x * NY + y] = ZUNPACK(zr)

    def push(src, dst, ssem, rsem, dy=None, dx=None):
        py = y if dy is None else lax.rem(y + dy, NY)
        px = x if dx is None else dx
        c = pltpu.make_async_remote_copy(
            src_ref=src, dst_ref=dst, send_sem=ssem, recv_sem=rsem,
            device_id={"tp": py * NX + px}, device_id_type=MESH,
        )
        c.start()

    def arrived(ref, rsem):
        pltpu.make_async_remote_copy(
            src_ref=ref, dst_ref=ref, send_sem=sx, recv_sem=rsem,
            device_id={"tp": lax.rem(t + 1, TP)}, device_id_type=MESH,
        ).wait_recv()

    mine = xf.at[x * NY + y]
    for d in (4, 3, 5, 2, 6, 1, 7):
        push(mine, mine, sx, rdy.at[d], dy=d)

    def at_y(off):
        return lax.rem(y + off, NY)

    def relay(k):
        yk = at_y(NEAR[k])
        if k % 2 == 0:
            ref = xf.at[xm * NY + yk]
            arrived(ref, rdl.at[k])
            push(ref, ref, sx, rdo.at[k], dx=xp)
        else:
            ref = xf.at[xp * NY + yk]
            arrived(ref, rdr.at[k])
            push(ref, ref, sx, rdo.at[k], dx=xm)

    for k in range(8):
        ref = xf.at[x * NY + at_y(NEAR[k])]
        if k > 0:
            arrived(ref, rdy.at[(8 - NEAR[k]) % 8])
        push(ref, ref, sx, rdl.at[k], dx=xp)
        push(ref, ref, sx, rdr.at[k], dx=xm)
        if k >= 3:
            relay(k - 3)
    for k in range(5, 8):
        relay(k)

    lo256 = lo_lanes(128, 256)

    def slab(xs, acc, ssq):
        for k in range(4):
            xa = xf[xs * NY + 2 * k].astype(F32)
            xb = xf[xs * NY + 2 * k + 1].astype(F32)
            ssq = ssq + xa * xa + xb * xb
            ta_i = 8 * k + xs
            tb_i = 8 * k + 4 + xs
            ga = gd2[xs % 2, pl.ds(4 * k + xs // 2, 1), :]
            gb = gd2[xs % 2, pl.ds(4 * k + 2 + xs // 2, 1), :]
            v = jnp.concatenate([xa * ga, xb * gb], axis=1)
            lhs = jnp.concatenate(
                [jnp.where(lo256, v, 0.0).astype(BF16), jnp.where(lo256, 0.0, v).astype(BF16)], axis=0
            )
            rhs = jnp.concatenate(
                [wi[ta_i].reshape(128, 256), wi[tb_i].reshape(128, 256)], axis=0
            )
            acc = acc + jnp.dot(lhs, rhs, preferred_element_type=F32)
        return acc, ssq

    acc = jnp.zeros((256, 256), F32)
    ssq = jnp.zeros((128, 128), F32)
    acc, ssq = slab(x, acc, ssq)
    for k in (1, 3, 5, 7):
        arrived(xf.at[xm * NY + at_y(NEAR[k])], rdl.at[k])
    acc, ssq = slab(xm, acc, ssq)
    for k in (0, 2, 4, 6):
        arrived(xf.at[xp * NY + at_y(NEAR[k])], rdr.at[k])
    acc, ssq = slab(xp, acc, ssq)
    for k in range(8):
        arrived(xf.at[xo * NY + at_y(NEAR[k])], rdo.at[k])
    acc, ssq = slab(xo, acc, ssq)

    s0 = jnp.sum(jnp.where(lo128, ssq, 0.0), axis=1, keepdims=True)
    s1 = jnp.sum(jnp.where(lo128, 0.0, ssq), axis=1, keepdims=True)
    scale = lax.rsqrt(jnp.concatenate([s0, s1], axis=0) / 2048.0 + EPS)
    gate, up = acc[:, 0:128] * scale, acc[:, 128:256] * scale
    hidden = (jax.nn.silu(gate) * up).astype(BF16)
    hid = jnp.concatenate([hidden[0:128], hidden[128:256]], axis=1)

    def share(xs, k):
        i = xs * NY + at_y(FAR[k])
        yf[i] = jnp.dot(hid, wd2[i], preferred_element_type=F32).astype(BF16)

    for k in range(8):
        share(xo, k)
        src = yf.at[xo * NY + at_y(FAR[k])]
        push(src, ro.at[k], se, reo.at[k], dx=xp if k % 2 == 0 else xm)
    for k in range(8):
        share(xp, k)
        share(xm, k)
        src_p, src_m = yf.at[xp * NY + at_y(FAR[k])], yf.at[xm * NY + at_y(FAR[k])]
        if k % 2 == 0:
            push(src_m, rr.at[k], se, rer.at[k], dx=xm)
        else:
            push(src_p, rl.at[k], se, rel.at[k], dx=xp)
    for k in range(8):
        i_p, i_m = xp * NY + at_y(FAR[k]), xm * NY + at_y(FAR[k])
        arrived(ro.at[k], reo.at[k])
        if k % 2 == 0:
            yf[i_p] = (yf[i_p].astype(F32) + ro[k].astype(F32)).astype(BF16)
            push(yf.at[i_p], rl.at[k], se, rel.at[k], dx=xp)
        else:
            yf[i_m] = (yf[i_m].astype(F32) + ro[k].astype(F32)).astype(BF16)
            push(yf.at[i_m], rr.at[k], se, rer.at[k], dx=xm)
    total = None
    for k in range(8):
        i = x * NY + at_y(FAR[k])
        own = jnp.dot(hid, wd2[i], preferred_element_type=F32)
        arrived(rl.at[k], rel.at[k])
        arrived(rr.at[k], rer.at[k])
        total = own + rl[k].astype(F32) + rr[k].astype(F32)
        if FAR[k] != 0:
            yf[i] = total.astype(BF16)
            push(yf.at[i], ry.at[FAR[k] - 1], se, rey.at[FAR[k] - 1], dy=FAR[k])
    for d in (1, 7, 2, 6, 3, 5, 4):
        arrived(ry.at[d - 1], rey.at[d - 1])
        total = total + ry[d - 1].astype(F32)

    ZPACK(qs, total)
    qr[e] = qs[e]
    to_ep(qs, qr, sq, rq)
    all_of(qr, sq, rq).wait_recv()
    back = ZUNPACK(qr).astype(F32)
    a0 = jnp.dot(wtv[0], back, precision=HI, preferred_element_type=F32)
    a1 = jnp.dot(wtv[1], back, precision=HI, preferred_element_type=F32)
    comb = jnp.where(lo64, a0, a1)
    out_ref[...] = (tokd[...] + (comb + swap(comb)))[:, 0:64].astype(BF16)

    all_of(ta, sa, ra).wait_send()
    all_of(wo, sw, rw_sem).wait_send()
    all_of(ma, sm, rm).wait_send()
    all_of(zs, sz, rz).wait_send()
    all_of(qs, sq, rq).wait_send()
    all_of(xf, sx, rz).wait_send()
    all_of(yf, se, rz).wait_send()


def ZPACK(ref, v):
    ref[...] = v.reshape(ZSHAPE).astype(BF16)


def ZUNPACK(ref):
    return ref[...].reshape(128, 128)


ZSHAPE = (32, 4, 128)


def local(
    tokens, mix_gain, w_in, a_real, a_imag, log_step, b_coef, output_coefficients, skip, w_out,
    state, ffn_gain, w_gate, w_up, w_down, expert_ids, route_weights,
):
    vm = pl.BlockSpec(memory_space=pltpu.VMEM)
    hbm = pl.BlockSpec(memory_space=pl.ANY)
    smem = pl.BlockSpec(memory_space=pltpu.SMEM)
    dma = pltpu.SemaphoreType.DMA
    V = pltpu.VMEM
    return pl.pallas_call(
        body,
        name="layer",
        out_shape=(
            jax.ShapeDtypeStruct(tokens.shape, BF16),
            jax.ShapeDtypeStruct(state.shape, F32),
        ),
        in_specs=[
            vm, vm, hbm, vm, vm, smem, vm, vm, vm, vm, vm, vm, hbm, hbm, hbm, vm, vm,
        ],
        out_specs=(vm, vm),
        scratch_shapes=[
            V((32, 32, 128), BF16),
            V((32, 16, 128), BF16),
            V((32, 16, 128), BF16),
            V((32, 16, 128), BF16),
            V(ZSHAPE, BF16),
            V(ZSHAPE, BF16),
            V((32, 128, 128), BF16),
            V((32, 128, 128), BF16),
            V((8, 128, 128), BF16),
            V((8, 128, 128), BF16),
            V((8, 128, 128), BF16),
            V((7, 128, 128), BF16),
            V(ZSHAPE, BF16),
            V(ZSHAPE, BF16),
            V((32, 2, 64, 32), BF16),
            V((32, 2, 64, 256), BF16),
            V((2, 128, 2048), BF16),
            V((32, 256, 128), BF16),
            V((2, 16, 128), F32),
            V((2, 16, 128), F32),
            V((128, 128), BF16),
            V((2, 64, 128), F32),
            V((64, 128), F32),
            dma((7,)),
            dma, dma, dma, dma, dma, dma, dma,
            dma, dma, dma, dma, dma,
            dma((8,)), dma((8,)), dma((8,)), dma((8,)),
            dma((8,)), dma((8,)), dma((8,)), dma((7,)),
        ],
        compiler_params=pltpu.CompilerParams(
            collective_id=0, has_side_effects=True, vmem_limit_bytes=48 * 1024 * 1024
        ),
    )(
        tokens, mix_gain.reshape(16, 128), w_in.reshape(32, 64, 32), a_real, a_imag, log_step,
        b_coef, output_coefficients, skip.reshape(1, 32), w_out, state, ffn_gain.reshape(16, 128),
        w_gate.reshape(2, 32, 64, 128), w_up.reshape(2, 32, 64, 128), w_down, expert_ids,
        route_weights,
    )


def solution(mesh):
    in_specs = (
        P("ep", "tp"), P(), P(None, "tp"), P("tp", None), P("tp", None), P("tp"),
        P(None, "tp", None, None), P(None, "tp", None, None), P("tp"), P("tp", None),
        P(None, "ep", "tp", None), P(), P("ep", None, "tp"), P("ep", None, "tp"),
        P("ep", "tp", None), P("ep", None), P("ep", None),
    )
    out_specs = (P("ep", "tp"), P(None, "ep", "tp", None))
    return jax.shard_map(local, mesh=mesh, in_specs=in_specs, out_specs=out_specs, check_vma=False)
```

```python
import jax
import jax.numpy as jnp
from jax import lax
from jax.experimental import pallas as pl
from jax.experimental.pallas import tpu as pltpu
from jax.sharding import PartitionSpec as P

EPS = 1e-06
HI = lax.Precision.HIGHEST
MESH = pl.DeviceIdType.MESH
NT = (((1,), (1,)), ((), ()))
TN = (((0,), (0,)), ((), ()))
F32 = jnp.float32
BF16 = jnp.bfloat16
NX, NY = 4, 8
TP, EP = 32, 32
NEAR = (0, 1, 7, 2, 6, 3, 5, 4)
FAR = (4, 3, 5, 2, 6, 1, 7, 0)


def iota(shape, dim):
    return lax.broadcasted_iota(jnp.int32, shape, dim)


def lo_lanes(rows, lanes=128):
    return iota((rows, lanes), 1) % 128 < 64


def swap(x):
    return pltpu.roll(x, 64, axis=x.ndim - 1)


def far_first(i):
    return 16 + ((i + 1) // 2) * (2 * (i % 2) - 1) * -1


def out_far(i):
    return 16 + ((i + 1) // 2) * (2 * (i % 2) - 1)


def out_near(i):
    return (1 - i % 2) * (8 - i // 2) - (i % 2) * (7 - i // 2)


def back_far(i):
    return 16 + ((i + 1) // 2) * (1 - 2 * (i % 2))


def back_near(i):
    return -out_near(i)


def body(
    tok_hbm, gain1_hbm, win_hbm, ar_hbm, ai_hbm, ls_hbm, b_hbm, oc_hbm, skip_hbm, wout_hbm,
    state_hbm, gain2_hbm, wg_hbm, wu_hbm, wd_hbm, ids_hbm, rw_hbm,
    out_hbm, ns_hbm, out_ref, ns_ref,
    tok_ref, gain1_ref, win_ref, ar_ref, ai_ref, ls_ref, b_ref, oc_ref, skip_ref, wout_ref,
    state_ref, gain2_ref, ids_ref, rw_ref,
    ta, ma, ws, wo, zs, zr, xf, yf, ro, rl, rr, ry, qs, qr, win2, wi, wdr, wd2,
    gd1, gd2, seltv, wtv, tokd,
    load_sem, put_sem, sa, sw, sv, sm, sz, sx, se, sq, ra, ray, rw_sem, rv, rm, rz, rq,
    rdy, rdl, rdr, rdo, reo, rel, rer, rey,
):
    t = lax.axis_index("tp")
    e = lax.axis_index("ep")
    y = t // NX
    x = t % NX
    xp = lax.rem(x + 1, NX)
    xm = lax.rem(x + NX - 1, NX)
    xo = lax.rem(x + 2, NX)

    loads = {}

    def load(name, src, dst):
        c = pltpu.make_async_copy(src, dst, load_sem.at[len(loads)])
        loads[name] = c
        c.start()

    load("tok", tok_hbm, tok_ref)
    load("wout", wout_hbm, wout_ref)
    barrier = pltpu.get_barrier_semaphore()

    def greet(i, c):
        d = far_first(i)
        pl.semaphore_signal(
            barrier, inc=1, device_id={"ep": lax.rem(e + d, EP)}, device_id_type=MESH
        )
        pl.semaphore_signal(
            barrier, inc=1, device_id={"tp": lax.rem(t + d, TP)}, device_id_type=MESH
        )
        return c

    lax.fori_loop(0, 31, greet, 0)
    load("ids", ids_hbm, ids_ref)
    load("rw", rw_hbm, rw_ref)
    load("gain1", gain1_hbm, gain1_ref)
    load("gain2", gain2_hbm, gain2_ref)
    load("win", win_hbm, win_ref)
    load("wd", wd_hbm, wdr)
    load("ar", ar_hbm, ar_ref)
    load("ai", ai_hbm, ai_ref)
    load("ls", ls_hbm, ls_ref)
    load("b", b_hbm, b_ref)
    load("oc", oc_hbm, oc_ref)
    load("skip", skip_hbm, skip_ref)
    load("state", state_hbm, state_ref)
    for j in range(2):
        load(f"g{j}", wg_hbm.at[j], wi.at[:, j, :, pl.ds(0, 128)])
        load(f"u{j}", wu_hbm.at[j], wi.at[:, j, :, pl.ds(128, 128)])
    loads["tok"].wait()

    tok = tok_ref[...]
    spread = (iota((64, 128), 1) % 64 == iota((64, 128), 0)).astype(F32)
    lo64 = lo_lanes(64)
    spread_lo = jnp.where(lo64, spread, 0.0).astype(BF16)
    spread_hi = jnp.where(lo64, 0.0, spread).astype(BF16)
    packed = jnp.dot(tok[0:32], spread_lo, preferred_element_type=F32) + jnp.dot(
        tok[32:64], spread_hi, preferred_element_type=F32
    )
    ta[t] = packed.astype(BF16)
    tokd[...] = jnp.dot(tok, spread.astype(BF16), preferred_element_type=F32)

    loads["wout"].wait()
    lo16 = lo_lanes(16)
    for k in range(16):
        blk = wout_ref[:, k * 128 : (k + 1) * 128].astype(F32)
        top, bot = blk[0:16], blk[16:32]
        ws[2 * k] = jnp.where(lo16, top, swap(bot)).astype(BF16)
        ws[2 * k + 1] = jnp.where(lo16, swap(top), bot).astype(BF16)
    @pl.when(y // 2 == lax.rem(e, 4))
    def _():
        wo[t] = ws[t]


    for name in ("ids", "rw", "gain1", "gain2", "win"):
        loads[name].wait()
    twice = spread.astype(BF16)
    ids = jnp.dot(
        ids_ref[...].astype(F32).astype(BF16), twice, preferred_element_type=F32
    ).astype(jnp.int32)
    rw = jnp.dot(rw_ref[...], spread, precision=HI, preferred_element_type=F32)
    slot = iota((128, 128), 0)
    named = 2 * (slot // 4) + iota((128, 128), 1) // 64
    hit0 = (ids[0:1] == named).astype(F32)
    hit1 = (ids[1:2] == named).astype(F32)
    hit = hit0 + hit1
    a_i, b_i = iota((128, 128), 0), iota((128, 128), 1)
    before = jnp.logical_and(a_i < b_i, a_i // 64 == b_i // 64).astype(F32).astype(BF16)
    rank = jnp.dot(hit.astype(BF16), before, preferred_element_type=F32)
    here = (rank.astype(jnp.int32) == slot % 4).astype(F32)
    seltv[...] = (hit * here).astype(BF16)
    wtv[...] = ((hit0 * rw[0:1] + hit1 * rw[1:2]) * here).T

    for src, dst in ((gain1_ref, gd1), (gain2_ref, gd2)):
        g = src[...]
        s = swap(g)
        lo = lo_lanes(16)
        dst[0] = jnp.where(lo, g, s)
        dst[1] = jnp.where(lo, s, g)

    lo32 = lo_lanes(32)
    for k in range(16):
        blk = win_ref[:, k * 128 : (k + 1) * 128].astype(F32)
        other = swap(blk)
        c = 256 * k
        win2[:, c : c + 128] = jnp.where(lo32, blk, other).astype(BF16)
        win2[:, c + 128 : c + 256] = jnp.where(lo32, other, blk).astype(BF16)
    loads["wd"].wait()
    lo128 = lo_lanes(128)
    for k in range(16):
        for j in range(2):
            blk = wdr[j, :, k * 128 : (k + 1) * 128].astype(F32)
            rolled = swap(blk)
            even, odd = (blk, rolled) if j == 0 else (rolled, blk)
            keep = lo128 if j == 0 else jnp.logical_not(lo128)
            for tt, piece in ((2 * k, even), (2 * k + 1, odd)):
                pos = (tt % NX) * NY + tt // NX
                wd2[pos, j * 128 : (j + 1) * 128, :] = jnp.where(keep, piece, 0.0).astype(BF16)
    pl.semaphore_wait(barrier, 62)

    def to_tp(src, dst, send, recv):
        def one(i, c):
            dest = lax.rem(t + far_first(i), TP)
            pltpu.make_async_remote_copy(
                src_ref=src(dest), dst_ref=dst, send_sem=send, recv_sem=recv,
                device_id={"tp": dest}, device_id_type=MESH,
            ).start()
            return c

        lax.fori_loop(0, 31, one, 0)

    def to_ep(ref_from, ref_to, count, shift, send, recv):
        def one(i, c):
            d = shift(i)
            dest = lax.rem(e + d + EP, EP)
            pltpu.make_async_remote_copy(
                src_ref=ref_from(dest, d), dst_ref=ref_to(d), send_sem=send, recv_sem=recv,
                device_id={"ep": dest}, device_id_type=MESH,
            ).start()
            return c

        lax.fori_loop(0, count, one, 0)

    def push(src, dst, ssem, rsem, dy=None, dx=None):
        py = y if dy is None else lax.rem(y + dy, NY)
        px = x if dx is None else dx
        pltpu.make_async_remote_copy(
            src_ref=src, dst_ref=dst, send_sem=ssem, recv_sem=rsem,
            device_id={"tp": py * NX + px}, device_id_type=MESH,
        ).start()

    def arrived(ref, rsem):
        pltpu.make_async_remote_copy(
            src_ref=ref, dst_ref=ref, send_sem=sx, recv_sem=rsem,
            device_id={"tp": lax.rem(t + 1, TP)}, device_id_type=MESH,
        ).wait_recv()

    def at_y(off):
        return lax.rem(y + off, NY)

    def offer(buf, ssem, ysem, xsem):
        ref = buf.at[t]
        for d in (4, 3, 5, 2, 6, 1, 7):
            push(ref, ref, ssem, ysem.at[d], dy=d)
        for px in (xo, xp, xm):
            push(ref, ref, ssem, xsem, dx=px)

    def pass_on(buf, ssem, ysem, xsem, between):
        for off in NEAR[1:]:
            ref = buf.at[at_y(off) * NX + x]
            arrived(ref, ysem.at[8 - off])
            for px in (xo, xp, xm):
                push(ref, ref, ssem, xsem, dx=px)
        between()
        arrived(buf.at[pl.ds(0, 24)], xsem)

    def all_of(ref, send, recv):
        r = ref.at[pl.ds(0, 31)]
        return pltpu.make_async_remote_copy(
            src_ref=r, dst_ref=r, send_sem=send, recv_sem=recv,
            device_id={"tp": lax.rem(t + 1, TP)}, device_id_type=MESH,
        )

    offer(ta, sa, ray, ra)
    row = lax.rem(e, 4)
    fetch = y // 2 == row

    @pl.when(fetch)
    def _():
        to_tp(lambda d: ws.at[d], wo.at[t], sw, rw_sem)


    for name in ("ar", "ai", "ls", "b", "oc", "skip", "state", "g0", "u0", "g1", "u1"):
        loads[name].wait()

    block = wo.at[pl.ds(row * 8, 8)]

    def share_projection():
        @pl.when(fetch)
        def _():
            arrived(wo.at[pl.ds(0, 7)], rw_sem)

        @pl.when(jnp.logical_not(fetch))
        def _():
            arrived(wo.at[pl.ds(0, 8)], rw_sem)

        for d in (2, 1, 3):
            pltpu.make_async_remote_copy(
                src_ref=block, dst_ref=block, send_sem=sv, recv_sem=rv,
                device_id={"ep": e - row + lax.rem(row + d, 4)}, device_id_type=MESH,
            ).start()

    pass_on(ta, sa, ray, ra, share_projection)
    acc = jnp.zeros((32, 128), F32)
    for k in range(TP):
        v = ta[k].astype(F32)
        acc = acc + v * v
    s0 = jnp.sum(jnp.where(lo32, acc, 0.0), axis=1, keepdims=True)
    s1 = jnp.sum(jnp.where(lo32, 0.0, acc), axis=1, keepdims=True)
    scale = jnp.where(
        lo32, lax.rsqrt(s0 / 2048.0 + EPS), lax.rsqrt(s1 / 2048.0 + EPS)
    )
    blocks = []
    for k in range(TP):
        v = ta[k].astype(F32) * scale * gd1[k % 2, k // 2 : k // 2 + 1, :]
        blocks.append(
            jnp.concatenate(
                [jnp.where(lo32, v, 0.0).astype(BF16), jnp.where(lo32, 0.0, v).astype(BF16)], axis=0
            )
        )
    drive = lax.dot_general(
        jnp.concatenate(blocks, axis=1), win2[...], NT, preferred_element_type=F32
    )
    drive = drive.astype(BF16).astype(F32)

    readout = skip_ref[...] * drive
    zeros16 = jnp.zeros((16, 64), F32)
    for g in range(2):
        step = jnp.exp(ls_ref[:, g : g + 1])
        ar, ai = ar_ref[g : g + 1, :], ai_ref[g : g + 1, :]
        mag = jnp.exp(step * ar)
        dr, di = mag * jnp.cos(step * ai), mag * jnp.sin(step * ai)
        den = ar * ar + ai * ai
        sh = dr - 1.0
        fr, fi = (sh * ar + di * ai) / den, (di * ar - sh * ai) / den
        u = drive[:, g * 16 : (g + 1) * 16]
        q0 = jnp.dot(u, b_ref[0, g], precision=HI, preferred_element_type=F32)
        q1 = jnp.dot(u, b_ref[1, g], precision=HI, preferred_element_type=F32)
        p0, p1 = state_ref[0, :, g, :], state_ref[1, :, g, :]
        n0 = dr * p0 - di * p1 + (fr * q0 - fi * q1)
        n1 = dr * p1 + di * p0 + (fr * q1 + fi * q0)
        ns_ref[0, :, g, :] = n0
        ns_ref[1, :, g, :] = n1
        order = (lambda o: [o, zeros16]) if g == 0 else (lambda o: [zeros16, o])
        c0 = jnp.concatenate(order(oc_ref[0, g]), axis=0)
        c1 = jnp.concatenate(order(oc_ref[1, g]), axis=0)
        readout = readout + (
            lax.dot_general(n0, c0, NT, precision=HI, preferred_element_type=F32)
            - lax.dot_general(n1, c1, NT, precision=HI, preferred_element_type=F32)
        )
    put_state = pltpu.make_async_copy(ns_ref, ns_hbm, put_sem.at[0])
    put_state.start()
    mixed = jax.nn.gelu(readout)
    first = iota((64, 32), 1) < 16
    stacked = jnp.concatenate(
        [jnp.where(first, mixed, 0.0), jnp.where(first, 0.0, mixed)], axis=0
    ).astype(BF16)
    pick = (iota((16, 32), 1) % 16 == iota((16, 32), 0)).astype(F32).astype(BF16)
    ma[t] = lax.dot_general(pick, stacked, NT, preferred_element_type=F32).astype(BF16)
    to_tp(lambda d: ma.at[t], ma.at[t], sm, rm)
    all_of(ma, sm, rm).wait_recv()
    arrived(wo.at[pl.ds(0, 24)], rv)
    prod = lax.dot_general(
        ma[...].reshape(512, 128), wo[...].reshape(512, 128), TN, preferred_element_type=F32
    )
    half = jnp.where(lo64, prod[0:64], prod[64:128])
    resid = (tokd[...] + (half + swap(half))).astype(BF16)
    resid_f = resid.astype(F32)
    tokd[...] = resid_f

    zero = jnp.zeros((64, 128), F32)
    diag = jnp.concatenate(
        [jnp.where(lo64, resid_f, zero), jnp.where(lo64, zero, resid_f)], axis=0
    ).astype(BF16)
    sent = jnp.dot(seltv[...], diag, preferred_element_type=F32)
    ZPACK(zs, sent)
    zr[8] = zs[e]
    for c, count, shift in ((1, 16, out_far), (0, 15, out_near)):
        to_ep(
            lambda dest, d: zs.at[dest], lambda d: zr.at[lax.rem(40 - d, EP)], count, shift, sz,
            rz.at[c],
        )

    def part(c, i):
        return xf.at[i, pl.ds(64 * c, 64)]

    def begin(c):
        arrived(zr.at[pl.ds(0, 15 + c)], rz.at[c])
        xf[x * NY + y, 64 * c : 64 * c + 64, :] = zr[16 * c : 16 * c + 16].reshape(64, 128)
        ref = part(c, x * NY + y)
        for d in (1, 7, 2, 6):
            push(ref, ref, sx, rdy.at[c, d], dy=d)
        push(ref, ref, sx, rdl.at[c, 0], dx=xp)
        push(ref, ref, sx, rdr.at[c, 0], dx=xm)

    def onward(c, k):
        ref = part(c, x * NY + at_y(NEAR[k]))
        arrived(ref, rdy.at[c, 8 - NEAR[k]])
        if NEAR[k] == 2:
            push(ref, ref, sx, rdy.at[c, 5], dy=7)
            if c == 0:
                push(ref, ref, sx, rdy.at[c, 4], dy=6)
        if NEAR[k] == 6:
            push(ref, ref, sx, rdy.at[c, 3], dy=1)
            if c == 1:
                push(ref, ref, sx, rdy.at[c, 4], dy=2)
        push(ref, ref, sx, rdl.at[c, k], dx=xp)
        push(ref, ref, sx, rdr.at[c, k], dx=xm)

    def relay(c, k):
        yk = at_y(NEAR[k])
        if k % 2 == 0:
            ref = part(c, xm * NY + yk)
            arrived(ref, rdl.at[c, k])
            push(ref, ref, sx, rdo.at[c, k], dx=xp)
        else:
            ref = part(c, xp * NY + yk)
            arrived(ref, rdr.at[c, k])
            push(ref, ref, sx, rdo.at[c, k], dx=xm)

    begin(0)
    for k in range(1, 5):
        onward(0, k)
    begin(1)
    for k in range(5, 8):
        onward(0, k)
        relay(0, k - 5)
    for k in range(1, 5):
        onward(1, k)
        relay(0, k + 2)
    relay(0, 7)
    for k in range(5, 8):
        onward(1, k)
        relay(1, k - 5)
    for k in range(3, 8):
        relay(1, k)

    lo256 = lo_lanes(128, 256)

    def slab(xs, acc, ssq):
        for k in range(4):
            xa = xf[xs * NY + 2 * k].astype(F32)
            xb = xf[xs * NY + 2 * k + 1].astype(F32)
            ssq = ssq + xa * xa + xb * xb
            ta_i = 8 * k + xs
            tb_i = 8 * k + 4 + xs
            ga = gd2[xs % 2, pl.ds(4 * k + xs // 2, 1), :]
            gb = gd2[xs % 2, pl.ds(4 * k + 2 + xs // 2, 1), :]
            v = jnp.concatenate([xa * ga, xb * gb], axis=1)
            lhs = jnp.concatenate(
                [jnp.where(lo256, v, 0.0).astype(BF16), jnp.where(lo256, 0.0, v).astype(BF16)], axis=0
            )
            rhs = jnp.concatenate(
                [wi[ta_i].reshape(128, 256), wi[tb_i].reshape(128, 256)], axis=0
            )
            acc = acc + jnp.dot(lhs, rhs, preferred_element_type=F32)
        return acc, ssq

    acc = jnp.zeros((256, 256), F32)
    ssq = jnp.zeros((128, 128), F32)
    acc, ssq = slab(x, acc, ssq)
    for c in range(2):
        for k in (1, 3, 5, 7):
            arrived(part(c, xm * NY + at_y(NEAR[k])), rdl.at[c, k])
    acc, ssq = slab(xm, acc, ssq)
    for c in range(2):
        for k in (0, 2, 4, 6):
            arrived(part(c, xp * NY + at_y(NEAR[k])), rdr.at[c, k])
    acc, ssq = slab(xp, acc, ssq)
    for c in range(2):
        for k in range(8):
            arrived(part(c, xo * NY + at_y(NEAR[k])), rdo.at[c, k])
    acc, ssq = slab(xo, acc, ssq)

    s0 = jnp.sum(jnp.where(lo128, ssq, 0.0), axis=1, keepdims=True)
    s1 = jnp.sum(jnp.where(lo128, 0.0, ssq), axis=1, keepdims=True)
    scale = lax.rsqrt(jnp.concatenate([s0, s1], axis=0) / 2048.0 + EPS)
    gate, up = acc[:, 0:128] * scale, acc[:, 128:256] * scale
    hidden = (jax.nn.silu(gate) * up).astype(BF16)
    hid = jnp.concatenate([hidden[0:128], hidden[128:256]], axis=1)

    def share(xs, k):
        i = xs * NY + at_y(FAR[k])
        yf[i] = jnp.dot(hid, wd2[i], preferred_element_type=F32).astype(BF16)

    def rows(ref, c, i):
        return ref.at[i, pl.ds(64 * c, 64)]

    def to_far(c, k):
        src = rows(yf, c, xo * NY + at_y(FAR[k]))
        push(src, rows(ro, c, k), se, reo.at[c, k], dx=xp if k % 2 == 0 else xm)

    def to_next(c, k):
        if k % 2 == 0:
            push(rows(yf, c, xm * NY + at_y(FAR[k])), rows(rr, c, k), se, rer.at[c, k], dx=xm)
        else:
            push(rows(yf, c, xp * NY + at_y(FAR[k])), rows(rl, c, k), se, rel.at[c, k], dx=xp)

    def add_on(c, k):
        r = slice(64 * c, 64 * c + 64)
        arrived(rows(ro, c, k), reo.at[c, k])
        px = xp if k % 2 == 0 else xm
        i = px * NY + at_y(FAR[k])
        yf[i, r, :] = (yf[i, r, :].astype(F32) + ro[k, r, :].astype(F32)).astype(BF16)
        if k % 2 == 0:
            push(rows(yf, c, i), rows(rl, c, k), se, rel.at[c, k], dx=xp)
        else:
            push(rows(yf, c, i), rows(rr, c, k), se, rer.at[c, k], dx=xm)

    def over_y(c):
        r = slice(64 * c, 64 * c + 64)
        for k in range(8):
            i = x * NY + at_y(FAR[k])
            arrived(rows(rl, c, k), rel.at[c, k])
            arrived(rows(rr, c, k), rer.at[c, k])
            total = yf[i, r, :].astype(F32) + rl[k, r, :].astype(F32) + rr[k, r, :].astype(F32)
            if FAR[k] != 0:
                yf[i, r, :] = total.astype(BF16)
                dst = rows(ry, c, FAR[k] - 1)
                push(rows(yf, c, i), dst, se, rey.at[c, FAR[k]], dy=FAR[k])
        return total

    def finish(c, total):
        r = slice(64 * c, 64 * c + 64)
        for d in (1, 7, 2, 6, 3, 5, 4):
            arrived(rows(ry, c, d - 1), rey.at[c, d])
            total = total + ry[d - 1, r, :].astype(F32)
        qs[16 * c : 16 * c + 16] = total.reshape(16, 4, 128).astype(BF16)
        count, shift = (15, back_near) if c == 0 else (16, back_far)
        to_ep(lambda dest, d: qs.at[d + 8], lambda d: qr.at[e], count, shift, sq, rq)

    for k in range(8):
        share(xo, k)
        to_far(1, k)
    for k in range(8):
        share(xp, k)
        share(xm, k)
        to_next(1, k)
    for k in range(8):
        to_far(0, k)
    for k in range(8):
        add_on(1, k)
    for k in range(8):
        to_next(0, k)
    for k in range(8):
        share(x, k)
    for k in range(8):
        add_on(0, k)
    total = over_y(1)
    near_total = over_y(0)
    finish(1, total)
    finish(0, near_total)

    qr[e] = qs[8]
    all_of(qr, sq, rq).wait_recv()
    back = ZUNPACK(qr).astype(F32)
    both = jnp.dot(wtv[...], back, precision=HI, preferred_element_type=F32)
    comb = jnp.where(lo64, both[0:64], both[64:128])
    out_ref[...] = (tokd[...] + (comb + swap(comb)))[:, 0:64].astype(BF16)
    put_out = pltpu.make_async_copy(out_ref, out_hbm, put_sem.at[1])
    put_out.start()

    all_of(ta, sa, ra).wait_send()

    @pl.when(fetch)
    def _():
        all_of(wo, sw, rw_sem).wait_send()

    blocks = wo.at[pl.ds(0, 24)]
    pltpu.make_async_remote_copy(
        src_ref=blocks, dst_ref=blocks, send_sem=sv, recv_sem=rv,
        device_id={"tp": lax.rem(t + 1, TP)}, device_id_type=MESH,
    ).wait_send()
    all_of(ma, sm, rm).wait_send()
    all_of(zs, sz, rq).wait_send()
    all_of(qs, sq, rq).wait_send()
    all_of(xf, sx, rq).wait_send()
    all_of(yf, se, rq).wait_send()
    put_state.wait()
    put_out.wait()


def ZPACK(ref, v):
    ref[...] = v.reshape(ZSHAPE).astype(BF16)


def ZUNPACK(ref):
    return ref[...].reshape(128, 128)


ZSHAPE = (32, 4, 128)


def local(
    tokens, mix_gain, w_in, a_real, a_imag, log_step, b_coef, output_coefficients, skip, w_out,
    state, ffn_gain, w_gate, w_up, w_down, expert_ids, route_weights,
):
    hbm = pl.BlockSpec(memory_space=pltpu.HBM)
    dma = pltpu.SemaphoreType.DMA
    V = pltpu.VMEM
    return pl.pallas_call(
        body,
        name="layer",
        out_shape=(
            jax.ShapeDtypeStruct(tokens.shape, BF16),
            jax.ShapeDtypeStruct(state.shape, F32),
        ),
        in_specs=[hbm] * 17,
        out_specs=(hbm, hbm),
        scratch_shapes=[
            V((64, 64), BF16),
            V((2, 64, 2, 64), F32),
            V((64, 64), BF16),
            V((16, 128), F32),
            V((32, 2048), BF16),
            V((2, 64), F32),
            V((2, 64), F32),
            V((1, 2), F32),
            V((2, 2, 16, 64), F32),
            V((2, 2, 16, 64), F32),
            V((1, 32), F32),
            V((32, 2048), BF16),
            V((2, 64, 2, 64), F32),
            V((16, 128), F32),
            V((2, 64), jnp.int32),
            V((2, 64), F32),
            V((32, 32, 128), BF16),
            V((32, 16, 128), BF16),
            V((32, 16, 128), BF16),
            V((32, 16, 128), BF16),
            V(ZSHAPE, BF16),
            V(ZSHAPE, BF16),
            V((32, 128, 128), BF16),
            V((32, 128, 128), BF16),
            V((8, 128, 128), BF16),
            V((8, 128, 128), BF16),
            V((8, 128, 128), BF16),
            V((7, 128, 128), BF16),
            V(ZSHAPE, BF16),
            V(ZSHAPE, BF16),
            V((32, 4096), BF16),
            V((32, 2, 64, 256), BF16),
            V((2, 128, 2048), BF16),
            V((32, 256, 128), BF16),
            V((2, 16, 128), F32),
            V((2, 16, 128), F32),
            V((128, 128), BF16),
            V((128, 128), F32),
            V((64, 128), F32),
            dma((19,)),
            dma((2,)),
            dma, dma, dma, dma, dma, dma, dma, dma,
            dma, dma((8,)), dma, dma, dma,
            dma((2,)), dma,
            dma((2, 8)), dma((2, 8)), dma((2, 8)), dma((2, 8)),
            dma((2, 8)), dma((2, 8)), dma((2, 8)), dma((2, 8)),
        ],
        compiler_params=pltpu.CompilerParams(
            collective_id=0, has_side_effects=True, vmem_limit_bytes=67043328
        ),
    )(
        tokens, mix_gain.reshape(16, 128), w_in.T, a_real, a_imag,
        log_step.reshape(1, 2), b_coef.transpose(0, 1, 3, 2), output_coefficients, skip.reshape(1, 32), w_out, state, ffn_gain.reshape(16, 128),
        w_gate.reshape(2, 32, 64, 128), w_up.reshape(2, 32, 64, 128), w_down, expert_ids.T,
        route_weights.T,
    )


def solution(mesh):
    in_specs = (
        P("ep", "tp"), P(), P(None, "tp"), P("tp", None), P("tp", None), P("tp"),
        P(None, "tp", None, None), P(None, "tp", None, None), P("tp"), P("tp", None),
        P(None, "ep", "tp", None), P(), P("ep", None, "tp"), P("ep", None, "tp"),
        P("ep", "tp", None), P("ep", None), P("ep", None),
    )
    out_specs = (P("ep", "tp"), P(None, "ep", "tp", None))
    return jax.shard_map(local, mesh=mesh, in_specs=in_specs, out_specs=out_specs, check_vma=False)
```

```python
import jax
import jax.numpy as jnp
from jax import lax
from jax.experimental import pallas as pl
from jax.experimental.pallas import tpu as pltpu
from jax.sharding import PartitionSpec as P

EPS = 1e-06
HI = lax.Precision.HIGHEST
MESH = pl.DeviceIdType.MESH
NT = (((1,), (1,)), ((), ()))
TN = (((0,), (0,)), ((), ()))
F32 = jnp.float32
BF16 = jnp.bfloat16
NX, NY = 4, 8
TP, EP = 32, 32
NEAR = (0, 1, 7, 2, 6, 3, 5, 4)
FAR = (4, 3, 5, 2, 6, 1, 7, 0)


def iota(shape, dim):
    return lax.broadcasted_iota(jnp.int32, shape, dim)


def lo_lanes(rows, lanes=128):
    return iota((rows, lanes), 1) % 128 < 64


def swap(x):
    return pltpu.roll(x, 64, axis=x.ndim - 1)


def far_first(i):
    return 16 + ((i + 1) // 2) * (2 * (i % 2) - 1) * -1


def out_far(i):
    return 16 + ((i + 1) // 2) * (2 * (i % 2) - 1)


def out_near(i):
    return (1 - i % 2) * (8 - i // 2) - (i % 2) * (7 - i // 2)


def back_far(i):
    return 16 + ((i + 1) // 2) * (1 - 2 * (i % 2))


def back_near(i):
    return -out_near(i)


def body(
    tok_hbm, gain1_hbm, win_hbm, ar_hbm, ai_hbm, ls_hbm, b_hbm, oc_hbm, skip_hbm, wout_hbm,
    state_hbm, gain2_hbm, wg_hbm, wu_hbm, wd_hbm, ids_hbm, rw_hbm,
    out_hbm, ns_hbm, out_ref, ns_ref,
    tok_ref, gain1_ref, win_ref, ar_ref, ai_ref, ls_ref, b_ref, oc_ref, skip_ref, wout_ref,
    state_ref, gain2_ref, ids_ref, rw_ref,
    ta, ma, ws, wo, zs, zr, xf, yf, ro, rl, rr, ry, qs, qr, win2, wi, wdr, wd2,
    gd1, gd2, seltv, wtv, tokd,
    load_sem, put_sem, sa, sw, sv, sm, sz, sx, se, sq, ra, ray, rw_sem, rv, rm, rz, rq,
    rdy, rdl, rdr, rdo, reo, rel, rer, rey,
):
    t = lax.axis_index("tp")
    e = lax.axis_index("ep")
    y = t // NX
    x = t % NX
    xp = lax.rem(x + 1, NX)
    xm = lax.rem(x + NX - 1, NX)
    xo = lax.rem(x + 2, NX)

    loads = {}

    def load(name, src, dst):
        c = pltpu.make_async_copy(src, dst, load_sem.at[len(loads)])
        loads[name] = c
        c.start()

    load("tok", tok_hbm, tok_ref)
    load("wout", wout_hbm, wout_ref)
    barrier = pltpu.get_barrier_semaphore()

    def greet(i, c):
        d = far_first(i)
        pl.semaphore_signal(
            barrier, inc=1, device_id={"ep": lax.rem(e + d, EP)}, device_id_type=MESH
        )
        pl.semaphore_signal(
            barrier, inc=1, device_id={"tp": lax.rem(t + d, TP)}, device_id_type=MESH
        )
        return c

    lax.fori_loop(0, 31, greet, 0)
    load("ids", ids_hbm, ids_ref)
    load("rw", rw_hbm, rw_ref)
    load("gain1", gain1_hbm, gain1_ref)
    load("gain2", gain2_hbm, gain2_ref)
    load("win", win_hbm, win_ref)
    load("wd", wd_hbm, wdr)
    load("ar", ar_hbm, ar_ref)
    load("ai", ai_hbm, ai_ref)
    load("ls", ls_hbm, ls_ref)
    load("b", b_hbm, b_ref)
    load("oc", oc_hbm, oc_ref)
    load("skip", skip_hbm, skip_ref)
    load("state", state_hbm, state_ref)
    for j in range(2):
        load(f"g{j}", wg_hbm.at[j], wi.at[:, j, :, pl.ds(0, 128)])
        load(f"u{j}", wu_hbm.at[j], wi.at[:, j, :, pl.ds(128, 128)])
    loads["tok"].wait()

    tok = tok_ref[...]
    spread = (iota((64, 128), 1) % 64 == iota((64, 128), 0)).astype(F32)
    lo64 = lo_lanes(64)
    spread_lo = jnp.where(lo64, spread, 0.0).astype(BF16)
    spread_hi = jnp.where(lo64, 0.0, spread).astype(BF16)
    packed = jnp.dot(tok[0:32], spread_lo, preferred_element_type=F32) + jnp.dot(
        tok[32:64], spread_hi, preferred_element_type=F32
    )
    ta[t] = packed.astype(BF16)
    tokd[...] = jnp.dot(tok, spread.astype(BF16), preferred_element_type=F32)

    loads["wout"].wait()
    lo16 = lo_lanes(16)
    for k in range(16):
        blk = wout_ref[:, k * 128 : (k + 1) * 128].astype(F32)
        top, bot = blk[0:16], blk[16:32]
        ws[2 * k] = jnp.where(lo16, top, swap(bot)).astype(BF16)
        ws[2 * k + 1] = jnp.where(lo16, swap(top), bot).astype(BF16)
    @pl.when(y // 2 == lax.rem(e, 4))
    def _():
        wo[t] = ws[t]


    for name in ("ids", "rw", "gain1", "gain2", "win"):
        loads[name].wait()
    twice = spread.astype(BF16)
    ids = jnp.dot(
        ids_ref[...].astype(F32).astype(BF16), twice, preferred_element_type=F32
    ).astype(jnp.int32)
    rw = jnp.dot(rw_ref[...], spread, precision=HI, preferred_element_type=F32)
    slot = iota((128, 128), 0)
    named = 2 * (slot // 4) + iota((128, 128), 1) // 64
    hit0 = (ids[0:1] == named).astype(F32)
    hit1 = (ids[1:2] == named).astype(F32)
    hit = hit0 + hit1
    a_i, b_i = iota((128, 128), 0), iota((128, 128), 1)
    before = jnp.logical_and(a_i < b_i, a_i // 64 == b_i // 64).astype(F32).astype(BF16)
    rank = jnp.dot(hit.astype(BF16), before, preferred_element_type=F32)
    here = (rank.astype(jnp.int32) == slot % 4).astype(F32)
    seltv[...] = (hit * here).astype(BF16)
    wtv[...] = ((hit0 * rw[0:1] + hit1 * rw[1:2]) * here).T

    for src, dst in ((gain1_ref, gd1), (gain2_ref, gd2)):
        g = src[...]
        s = swap(g)
        lo = lo_lanes(16)
        dst[0] = jnp.where(lo, g, s)
        dst[1] = jnp.where(lo, s, g)

    lo32 = lo_lanes(32)
    for k in range(16):
        blk = win_ref[:, k * 128 : (k + 1) * 128].astype(F32)
        other = swap(blk)
        c = 256 * k
        win2[:, c : c + 128] = jnp.where(lo32, blk, other).astype(BF16)
        win2[:, c + 128 : c + 256] = jnp.where(lo32, other, blk).astype(BF16)
    loads["wd"].wait()
    lo128 = lo_lanes(128)
    for k in range(16):
        for j in range(2):
            blk = wdr[j, :, k * 128 : (k + 1) * 128].astype(F32)
            rolled = swap(blk)
            even, odd = (blk, rolled) if j == 0 else (rolled, blk)
            keep = lo128 if j == 0 else jnp.logical_not(lo128)
            for tt, piece in ((2 * k, even), (2 * k + 1, odd)):
                pos = (tt % NX) * NY + tt // NX
                wd2[pos, j * 128 : (j + 1) * 128, :] = jnp.where(keep, piece, 0.0).astype(BF16)
    pl.semaphore_wait(barrier, 62)

    def to_tp(src, dst, send, recv):
        def one(i, c):
            dest = lax.rem(t + far_first(i), TP)
            pltpu.make_async_remote_copy(
                src_ref=src(dest), dst_ref=dst, send_sem=send, recv_sem=recv,
                device_id={"tp": dest}, device_id_type=MESH,
            ).start()
            return c

        lax.fori_loop(0, 31, one, 0)

    def to_ep(ref_from, ref_to, count, shift, send, recv):
        def one(i, c):
            d = shift(i)
            dest = lax.rem(e + d + EP, EP)
            pltpu.make_async_remote_copy(
                src_ref=ref_from(dest, d), dst_ref=ref_to(d), send_sem=send, recv_sem=recv,
                device_id={"ep": dest}, device_id_type=MESH,
            ).start()
            return c

        lax.fori_loop(0, count, one, 0)

    def push(src, dst, ssem, rsem, dy=None, dx=None):
        py = y if dy is None else lax.rem(y + dy, NY)
        px = x if dx is None else dx
        pltpu.make_async_remote_copy(
            src_ref=src, dst_ref=dst, send_sem=ssem, recv_sem=rsem,
            device_id={"tp": py * NX + px}, device_id_type=MESH,
        ).start()

    def arrived(ref, rsem):
        pltpu.make_async_remote_copy(
            src_ref=ref, dst_ref=ref, send_sem=sx, recv_sem=rsem,
            device_id={"tp": lax.rem(t + 1, TP)}, device_id_type=MESH,
        ).wait_recv()

    def at_y(off):
        return lax.rem(y + off, NY)

    def offer(buf, ssem, ysem, xsem):
        ref = buf.at[t]
        for d in (4, 3, 5, 2, 6, 1, 7):
            push(ref, ref, ssem, ysem.at[d], dy=d)
        for px in (xo, xp, xm):
            push(ref, ref, ssem, xsem, dx=px)

    def pass_on(buf, ssem, ysem, xsem, between):
        for off in NEAR[1:]:
            ref = buf.at[at_y(off) * NX + x]
            arrived(ref, ysem.at[8 - off])
            for px in (xo, xp, xm):
                push(ref, ref, ssem, xsem, dx=px)
        between()
        arrived(buf.at[pl.ds(0, 24)], xsem)

    def all_of(ref, send, recv):
        r = ref.at[pl.ds(0, 31)]
        return pltpu.make_async_remote_copy(
            src_ref=r, dst_ref=r, send_sem=send, recv_sem=recv,
            device_id={"tp": lax.rem(t + 1, TP)}, device_id_type=MESH,
        )

    offer(ta, sa, ray, ra)
    row = lax.rem(e, 4)
    fetch = y // 2 == row

    @pl.when(fetch)
    def _():
        to_tp(lambda d: ws.at[d], wo.at[t], sw, rw_sem)


    for name in ("ar", "ai", "ls", "b", "oc", "skip", "state", "g0", "u0", "g1", "u1"):
        loads[name].wait()

    block = wo.at[pl.ds(row * 8, 8)]

    def share_projection():
        @pl.when(fetch)
        def _():
            arrived(wo.at[pl.ds(0, 7)], rw_sem)

        @pl.when(jnp.logical_not(fetch))
        def _():
            arrived(wo.at[pl.ds(0, 8)], rw_sem)

        for d in (2, 1, 3):
            pltpu.make_async_remote_copy(
                src_ref=block, dst_ref=block, send_sem=sv, recv_sem=rv,
                device_id={"ep": e - row + lax.rem(row + d, 4)}, device_id_type=MESH,
            ).start()

    pass_on(ta, sa, ray, ra, share_projection)
    acc = jnp.zeros((32, 128), F32)
    for k in range(TP):
        v = ta[k].astype(F32)
        acc = acc + v * v
    s0 = jnp.sum(jnp.where(lo32, acc, 0.0), axis=1, keepdims=True)
    s1 = jnp.sum(jnp.where(lo32, 0.0, acc), axis=1, keepdims=True)
    scale = jnp.where(
        lo32, lax.rsqrt(s0 / 2048.0 + EPS), lax.rsqrt(s1 / 2048.0 + EPS)
    )
    blocks = []
    for k in range(TP):
        v = ta[k].astype(F32) * scale * gd1[k % 2, k // 2 : k // 2 + 1, :]
        blocks.append(
            jnp.concatenate(
                [jnp.where(lo32, v, 0.0).astype(BF16), jnp.where(lo32, 0.0, v).astype(BF16)], axis=0
            )
        )
    drive = lax.dot_general(
        jnp.concatenate(blocks, axis=1), win2[...], NT, preferred_element_type=F32
    )
    drive = drive.astype(BF16).astype(F32)

    readout = skip_ref[...] * drive
    zeros16 = jnp.zeros((16, 64), F32)
    for g in range(2):
        step = jnp.exp(ls_ref[:, g : g + 1])
        ar, ai = ar_ref[g : g + 1, :], ai_ref[g : g + 1, :]
        mag = jnp.exp(step * ar)
        dr, di = mag * jnp.cos(step * ai), mag * jnp.sin(step * ai)
        den = ar * ar + ai * ai
        sh = dr - 1.0
        fr, fi = (sh * ar + di * ai) / den, (di * ar - sh * ai) / den
        u = drive[:, g * 16 : (g + 1) * 16]
        q0 = jnp.dot(u, b_ref[0, g], precision=HI, preferred_element_type=F32)
        q1 = jnp.dot(u, b_ref[1, g], precision=HI, preferred_element_type=F32)
        p0, p1 = state_ref[0, :, g, :], state_ref[1, :, g, :]
        n0 = dr * p0 - di * p1 + (fr * q0 - fi * q1)
        n1 = dr * p1 + di * p0 + (fr * q1 + fi * q0)
        ns_ref[0, :, g, :] = n0
        ns_ref[1, :, g, :] = n1
        order = (lambda o: [o, zeros16]) if g == 0 else (lambda o: [zeros16, o])
        c0 = jnp.concatenate(order(oc_ref[0, g]), axis=0)
        c1 = jnp.concatenate(order(oc_ref[1, g]), axis=0)
        readout = readout + (
            lax.dot_general(n0, c0, NT, precision=HI, preferred_element_type=F32)
            - lax.dot_general(n1, c1, NT, precision=HI, preferred_element_type=F32)
        )
    put_state = pltpu.make_async_copy(ns_ref, ns_hbm, put_sem.at[0])
    put_state.start()
    mixed = jax.nn.gelu(readout)
    first = iota((64, 32), 1) < 16
    stacked = jnp.concatenate(
        [jnp.where(first, mixed, 0.0), jnp.where(first, 0.0, mixed)], axis=0
    ).astype(BF16)
    pick = (iota((16, 32), 1) % 16 == iota((16, 32), 0)).astype(F32).astype(BF16)
    ma[t] = lax.dot_general(pick, stacked, NT, preferred_element_type=F32).astype(BF16)
    to_tp(lambda d: ma.at[t], ma.at[t], sm, rm)
    all_of(ma, sm, rm).wait_recv()
    arrived(wo.at[pl.ds(0, 24)], rv)
    prod = lax.dot_general(
        ma[...].reshape(512, 128), wo[...].reshape(512, 128), TN, preferred_element_type=F32
    )
    half = jnp.where(lo64, prod[0:64], prod[64:128])
    resid = (tokd[...] + (half + swap(half))).astype(BF16)
    resid_f = resid.astype(F32)
    tokd[...] = resid_f

    zero = jnp.zeros((64, 128), F32)
    diag = jnp.concatenate(
        [jnp.where(lo64, resid_f, zero), jnp.where(lo64, zero, resid_f)], axis=0
    ).astype(BF16)
    sent = jnp.dot(seltv[...], diag, preferred_element_type=F32)
    ZPACK(zs, sent)
    zr[8] = zs[e]
    for c, count, shift in ((1, 16, out_far), (0, 15, out_near)):
        to_ep(
            lambda dest, d: zs.at[dest], lambda d: zr.at[lax.rem(40 - d, EP)], count, shift, sz,
            rz.at[c],
        )

    def part(c, i):
        return xf.at[i, pl.ds(64 * c, 64)]

    def begin(c):
        arrived(zr.at[pl.ds(0, 15 + c)], rz.at[c])
        xf[x * NY + y, 64 * c : 64 * c + 64, :] = zr[16 * c : 16 * c + 16].reshape(64, 128)
        ref = part(c, x * NY + y)
        for d in (1, 7, 4, 3, 5, 2, 6):
            push(ref, ref, sx, rdy.at[c, d], dy=d)
        push(ref, ref, sx, rdl.at[c, 0], dx=xp)
        push(ref, ref, sx, rdr.at[c, 0], dx=xm)

    def onward(c, k):
        ref = part(c, x * NY + at_y(NEAR[k]))
        arrived(ref, rdy.at[c, 8 - NEAR[k]])
        push(ref, ref, sx, rdl.at[c, k], dx=xp)
        push(ref, ref, sx, rdr.at[c, k], dx=xm)

    def relay(c, k):
        yk = at_y(NEAR[k])
        if k % 2 == 0:
            ref = part(c, xm * NY + yk)
            arrived(ref, rdl.at[c, k])
            push(ref, ref, sx, rdo.at[c, k], dx=xp)
        else:
            ref = part(c, xp * NY + yk)
            arrived(ref, rdr.at[c, k])
            push(ref, ref, sx, rdo.at[c, k], dx=xm)

    begin(0)
    for k in range(1, 5):
        onward(0, k)
    begin(1)
    for k in range(5, 8):
        onward(0, k)
        relay(0, k - 5)
    for k in range(1, 5):
        onward(1, k)
        relay(0, k + 2)
    relay(0, 7)
    for k in range(5, 8):
        onward(1, k)
        relay(1, k - 5)
    for k in range(3, 8):
        relay(1, k)

    lo256 = lo_lanes(128, 256)

    def slab(xs, acc, ssq):
        for k in range(4):
            xa = xf[xs * NY + 2 * k].astype(F32)
            xb = xf[xs * NY + 2 * k + 1].astype(F32)
            ssq = ssq + xa * xa + xb * xb
            ta_i = 8 * k + xs
            tb_i = 8 * k + 4 + xs
            ga = gd2[xs % 2, pl.ds(4 * k + xs // 2, 1), :]
            gb = gd2[xs % 2, pl.ds(4 * k + 2 + xs // 2, 1), :]
            v = jnp.concatenate([xa * ga, xb * gb], axis=1)
            lhs = jnp.concatenate(
                [jnp.where(lo256, v, 0.0).astype(BF16), jnp.where(lo256, 0.0, v).astype(BF16)], axis=0
            )
            rhs = jnp.concatenate(
                [wi[ta_i].reshape(128, 256), wi[tb_i].reshape(128, 256)], axis=0
            )
            acc = acc + jnp.dot(lhs, rhs, preferred_element_type=F32)
        return acc, ssq

    acc = jnp.zeros((256, 256), F32)
    ssq = jnp.zeros((128, 128), F32)
    acc, ssq = slab(x, acc, ssq)
    for c in range(2):
        for k in (1, 3, 5, 7):
            arrived(part(c, xm * NY + at_y(NEAR[k])), rdl.at[c, k])
    acc, ssq = slab(xm, acc, ssq)
    for c in range(2):
        for k in (0, 2, 4, 6):
            arrived(part(c, xp * NY + at_y(NEAR[k])), rdr.at[c, k])
    acc, ssq = slab(xp, acc, ssq)
    for c in range(2):
        for k in range(8):
            arrived(part(c, xo * NY + at_y(NEAR[k])), rdo.at[c, k])
    acc, ssq = slab(xo, acc, ssq)

    s0 = jnp.sum(jnp.where(lo128, ssq, 0.0), axis=1, keepdims=True)
    s1 = jnp.sum(jnp.where(lo128, 0.0, ssq), axis=1, keepdims=True)
    scale = lax.rsqrt(jnp.concatenate([s0, s1], axis=0) / 2048.0 + EPS)
    gate, up = acc[:, 0:128] * scale, acc[:, 128:256] * scale
    hidden = (jax.nn.silu(gate) * up).astype(BF16)
    hid = jnp.concatenate([hidden[0:128], hidden[128:256]], axis=1)

    def share(xs, k):
        i = xs * NY + at_y(FAR[k])
        yf[i] = jnp.dot(hid, wd2[i], preferred_element_type=F32).astype(BF16)

    def rows(ref, c, i):
        return ref.at[i, pl.ds(64 * c, 64)]

    def to_far(c, k):
        src = rows(yf, c, xo * NY + at_y(FAR[k]))
        push(src, rows(ro, c, k), se, reo.at[c, k], dx=xp if k % 2 == 0 else xm)

    def to_next(c, k):
        if k % 2 == 0:
            push(rows(yf, c, xm * NY + at_y(FAR[k])), rows(rr, c, k), se, rer.at[c, k], dx=xm)
        else:
            push(rows(yf, c, xp * NY + at_y(FAR[k])), rows(rl, c, k), se, rel.at[c, k], dx=xp)

    def add_on(c, k):
        r = slice(64 * c, 64 * c + 64)
        arrived(rows(ro, c, k), reo.at[c, k])
        px = xp if k % 2 == 0 else xm
        i = px * NY + at_y(FAR[k])
        yf[i, r, :] = (yf[i, r, :].astype(F32) + ro[k, r, :].astype(F32)).astype(BF16)
        if k % 2 == 0:
            push(rows(yf, c, i), rows(rl, c, k), se, rel.at[c, k], dx=xp)
        else:
            push(rows(yf, c, i), rows(rr, c, k), se, rer.at[c, k], dx=xm)

    def over_y(c):
        r = slice(64 * c, 64 * c + 64)
        for k in range(8):
            i = x * NY + at_y(FAR[k])
            arrived(rows(rl, c, k), rel.at[c, k])
            arrived(rows(rr, c, k), rer.at[c, k])
            total = yf[i, r, :].astype(F32) + rl[k, r, :].astype(F32) + rr[k, r, :].astype(F32)
            if FAR[k] != 0:
                yf[i, r, :] = total.astype(BF16)
                dst = rows(ry, c, FAR[k] - 1)
                push(rows(yf, c, i), dst, se, rey.at[c, FAR[k]], dy=FAR[k])
        return total

    def finish(c, total):
        r = slice(64 * c, 64 * c + 64)
        for d in (1, 7, 2, 6, 3, 5, 4):
            arrived(rows(ry, c, d - 1), rey.at[c, d])
            total = total + ry[d - 1, r, :].astype(F32)
        qs[16 * c : 16 * c + 16] = total.reshape(16, 4, 128).astype(BF16)
        count, shift = (15, back_near) if c == 0 else (16, back_far)
        to_ep(lambda dest, d: qs.at[d + 8], lambda d: qr.at[e], count, shift, sq, rq)

    for k in range(8):
        share(xo, k)
        to_far(1, k)
    for k in range(8):
        share(xp, k)
        share(xm, k)
        to_next(1, k)
    for k in range(8):
        to_far(0, k)
    for k in range(8):
        add_on(1, k)
    for k in range(8):
        to_next(0, k)
    for k in range(8):
        share(x, k)
    for k in range(8):
        add_on(0, k)
    total = over_y(1)
    near_total = over_y(0)
    finish(1, total)
    finish(0, near_total)

    qr[e] = qs[8]
    all_of(qr, sq, rq).wait_recv()
    back = ZUNPACK(qr).astype(F32)
    both = jnp.dot(wtv[...], back, precision=HI, preferred_element_type=F32)
    comb = jnp.where(lo64, both[0:64], both[64:128])
    out_ref[...] = (tokd[...] + (comb + swap(comb)))[:, 0:64].astype(BF16)
    put_out = pltpu.make_async_copy(out_ref, out_hbm, put_sem.at[1])
    put_out.start()

    all_of(ta, sa, ra).wait_send()

    @pl.when(fetch)
    def _():
        all_of(wo, sw, rw_sem).wait_send()

    blocks = wo.at[pl.ds(0, 24)]
    pltpu.make_async_remote_copy(
        src_ref=blocks, dst_ref=blocks, send_sem=sv, recv_sem=rv,
        device_id={"tp": lax.rem(t + 1, TP)}, device_id_type=MESH,
    ).wait_send()
    all_of(ma, sm, rm).wait_send()
    all_of(zs, sz, rq).wait_send()
    all_of(qs, sq, rq).wait_send()
    all_of(xf, sx, rq).wait_send()
    all_of(yf, se, rq).wait_send()
    put_state.wait()
    put_out.wait()


def ZPACK(ref, v):
    ref[...] = v.reshape(ZSHAPE).astype(BF16)


def ZUNPACK(ref):
    return ref[...].reshape(128, 128)


ZSHAPE = (32, 4, 128)


def local(
    tokens, mix_gain, w_in, a_real, a_imag, log_step, b_coef, output_coefficients, skip, w_out,
    state, ffn_gain, w_gate, w_up, w_down, expert_ids, route_weights,
):
    hbm = pl.BlockSpec(memory_space=pltpu.HBM)
    dma = pltpu.SemaphoreType.DMA
    V = pltpu.VMEM
    return pl.pallas_call(
        body,
        name="layer",
        out_shape=(
            jax.ShapeDtypeStruct(tokens.shape, BF16),
            jax.ShapeDtypeStruct(state.shape, F32),
        ),
        in_specs=[hbm] * 17,
        out_specs=(hbm, hbm),
        scratch_shapes=[
            V((64, 64), BF16),
            V((2, 64, 2, 64), F32),
            V((64, 64), BF16),
            V((16, 128), F32),
            V((32, 2048), BF16),
            V((2, 64), F32),
            V((2, 64), F32),
            V((1, 2), F32),
            V((2, 2, 16, 64), F32),
            V((2, 2, 16, 64), F32),
            V((1, 32), F32),
            V((32, 2048), BF16),
            V((2, 64, 2, 64), F32),
            V((16, 128), F32),
            V((2, 64), jnp.int32),
            V((2, 64), F32),
            V((32, 32, 128), BF16),
            V((32, 16, 128), BF16),
            V((32, 16, 128), BF16),
            V((32, 16, 128), BF16),
            V(ZSHAPE, BF16),
            V(ZSHAPE, BF16),
            V((32, 128, 128), BF16),
            V((32, 128, 128), BF16),
            V((8, 128, 128), BF16),
            V((8, 128, 128), BF16),
            V((8, 128, 128), BF16),
            V((7, 128, 128), BF16),
            V(ZSHAPE, BF16),
            V(ZSHAPE, BF16),
            V((32, 4096), BF16),
            V((32, 2, 64, 256), BF16),
            V((2, 128, 2048), BF16),
            V((32, 256, 128), BF16),
            V((2, 16, 128), F32),
            V((2, 16, 128), F32),
            V((128, 128), BF16),
            V((128, 128), F32),
            V((64, 128), F32),
            dma((19,)),
            dma((2,)),
            dma, dma, dma, dma, dma, dma, dma, dma,
            dma, dma((8,)), dma, dma, dma,
            dma((2,)), dma,
            dma((2, 8)), dma((2, 8)), dma((2, 8)), dma((2, 8)),
            dma((2, 8)), dma((2, 8)), dma((2, 8)), dma((2, 8)),
        ],
        compiler_params=pltpu.CompilerParams(
            collective_id=0, has_side_effects=True, vmem_limit_bytes=67043328
        ),
    )(
        tokens, mix_gain.reshape(16, 128), w_in.T, a_real, a_imag,
        log_step.reshape(1, 2), b_coef.transpose(0, 1, 3, 2), output_coefficients, skip.reshape(1, 32), w_out, state, ffn_gain.reshape(16, 128),
        w_gate.reshape(2, 32, 64, 128), w_up.reshape(2, 32, 64, 128), w_down, expert_ids.T,
        route_weights.T,
    )


def solution(mesh):
    in_specs = (
        P("ep", "tp"), P(), P(None, "tp"), P("tp", None), P("tp", None), P("tp"),
        P(None, "tp", None, None), P(None, "tp", None, None), P("tp"), P("tp", None),
        P(None, "ep", "tp", None), P(), P("ep", None, "tp"), P("ep", None, "tp"),
        P("ep", "tp", None), P("ep", None), P("ep", None),
    )
    out_specs = (P("ep", "tp"), P(None, "ep", "tp", None))
    return jax.shard_map(local, mesh=mesh, in_specs=in_specs, out_specs=out_specs, check_vma=False)
```
